32 devices in a mesh: sp: 8 (over z, x), tp: 4 (over y, core).
Axes of the slice: x: 2, y: 2, z: 4, core: 2. Of those that a mesh axis runs over, the one named last changes fastest.
Arguments:
- queries: bfloat16 [1024, 1024], P('sp', 'tp'), may hold values from -12 to 12
- keys: bfloat16 [1024, 256], P('sp', 'tp'), may hold values from -12 to 12
- values: bfloat16 [1024, 256], P('sp', 'tp'), may hold values from -6 to 6
- log_gate: float32 [16, 1024], P('tp', 'sp'), may hold values from -0.2 to 0, as said below
- log_sum: float32 [16, 1024], P('tp', 'sp'), may hold values from -100 to 100, as said below
- output: bfloat16 [1024, 1024], P('sp', 'tp'), may hold values from -6 to 6
- cotangent: bfloat16 [1024, 1024], P('sp', 'tp'), may hold values from -12 to 12
- normed: bfloat16 [1024, 2048], P('sp', 'tp'), may hold values from -8 to 8
Outputs:
- query_grad: bfloat16 [1024, 1024], P('sp', 'tp')
- key_grad: bfloat16 [1024, 256], P('sp', 'tp')
- value_grad: bfloat16 [1024, 256], P('sp', 'tp')
- weight_grad: float32 [2048, 256], P('sp', 'tp')
The draws below stay inside these ranges and needn't reach their ends.
Inputs may be any that keep to these rules, and one draw needn't show every extreme that they name: `log_gate`: every entry is negative. log_sum[h, t] is the logarithm of the sum over s <= t of exp of the scores of the steps (before log_sum is subtracted), computed from the given queries, keys and log_gate.
All inputs are finite; a program needn't handle non-finite values.
Results may differ from the reference program's by a relative error of at most 0.005.
Values may be sent and summed in bfloat16 or wider, within the bound.
A program may use at most 64 MiB of HBM per device.

```python
import math
import jax
import jax.numpy as jnp
from jax import lax

D = 2048
HEADS = 16
KV_HEADS = 4
HDIM = 64
TOK_DEV = 128
SEQ = 1024


def make_gates(key):
    streams = jax.random.split(jax.random.fold_in(key, 11), 5)
    order = jax.random.permutation(streams[0], HEADS)
    lasting = order < HEADS // 2
    slow_rate = jax.random.uniform(streams[1], (HEADS,), jnp.float32, 0.3, 1.5) / SEQ
    fast_rate = jnp.exp(jax.random.uniform(streams[2], (HEADS,), jnp.float32, math.log(0.01), math.log(1.0 / 30.0)))
    rates = jnp.where(lasting, slow_rate, fast_rate)
    factors = jnp.exp(jax.random.uniform(streams[3], (HEADS, SEQ // TOK_DEV), jnp.float32, -0.7, 0.7))
    factors = jnp.repeat(factors, TOK_DEV, axis=1)
    rough = jax.random.uniform(streams[4], (HEADS, SEQ), jnp.float32, 0.5, 1.5)
    return -rates[:, None] * factors * rough


def make_queries(key):
    drawn = jax.random.normal(jax.random.fold_in(key, 21), (SEQ, HEADS * HDIM), jnp.float32)
    return jnp.clip(drawn, -12.0, 12.0).astype(jnp.bfloat16)


def make_keys(key):
    drawn = jax.random.normal(jax.random.fold_in(key, 31), (SEQ, KV_HEADS * HDIM), jnp.float32)
    return jnp.clip(drawn, -12.0, 12.0).astype(jnp.bfloat16)


def draw_queries(key, part):
    return make_queries(key)


def draw_keys(key, part):
    return make_keys(key)


def draw_log_gate(key, part):
    return make_gates(key)


def draw_log_sum(key, part):
    group_size = HEADS // KV_HEADS
    block_count = SEQ // TOK_DEV
    inverse_root = HDIM ** (-0.5)
    query_float = make_queries(key).astype(jnp.float32).reshape(block_count, TOK_DEV, KV_HEADS, group_size, HDIM)
    query_float = jnp.transpose(query_float, (2, 0, 1, 3, 4))
    key_float = jnp.transpose(make_keys(key).astype(jnp.float32).reshape(SEQ, KV_HEADS, HDIM), (1, 0, 2))
    cumulative = jnp.cumsum(make_gates(key), axis=1)
    cum_blocks = jnp.transpose(cumulative.reshape(KV_HEADS, group_size, block_count, TOK_DEV), (0, 2, 1, 3))
    cum_keys = cumulative.reshape(KV_HEADS, group_size, SEQ)
    key_positions = jnp.arange(SEQ)

    def one_group(inputs):
        query_group, cum_group, key_group, key_cum = inputs

        def one_block(pieces):
            query_block, cum_block, block_index = pieces
            query_positions = block_index * TOK_DEV + jnp.arange(TOK_DEV)
            scores = jnp.einsum('qgd,kd->gqk', query_block, key_group, precision=lax.Precision.HIGHEST) * inverse_root
            scores = scores + cum_block[:, :, None] - key_cum[:, None, :]
            allowed = key_positions[None, :] <= query_positions[:, None]
            scores = jnp.where(allowed[None], scores, -jnp.inf)
            return jax.nn.logsumexp(scores, axis=2)
        return lax.map(one_block, (query_group, cum_group, jnp.arange(block_count)))
    sums = lax.map(one_group, (query_float, cum_blocks, key_float, cum_keys))
    return jnp.transpose(sums, (0, 2, 1, 3)).reshape(HEADS, SEQ)


def spiked(values, rng, source, target, blocks, factor):
    owner, partner = [(jnp.arange(values.shape[position]) // (values.shape[position] // blocks)).reshape([-1 if axis == position else 1 for axis in range(values.ndim)]) for position in (source, target)]
    chosen = jax.random.permutation(rng, blocks)[partner]
    strong = (owner == chosen) | (owner == (partner + blocks // 2) % blocks)
    return jnp.where(strong, factor * values, values)


def shard_levels(key, dims, cuts, low, high):
    def one(axis_at, shards_of):
        draws = jax.random.uniform(jax.random.fold_in(jax.random.fold_in(key, 6), axis_at), (shards_of,), jnp.float32, low / len(cuts), high / len(cuts))
        return jnp.repeat(jnp.exp(draws), dims[axis_at] // shards_of).reshape((-1,) + (1,) * (len(dims) - axis_at - 1))

    loudness = one(*cuts[0])
    for cut in cuts[1:]:
        loudness = loudness * one(*cut)
    return loudness


def scatter_about(own_key, shape, spread, bound, cuts=(), kind=jnp.bfloat16):
    loudness = shard_levels(own_key, shape, cuts, -0.22, 0.18) if cuts else 1.0
    values = jax.random.normal(own_key, shape, jnp.float32) * spread * loudness
    return jnp.minimum(jnp.maximum(values, -bound), bound).astype(kind)


def noise_with(own_key, shape, spread, limit, cuts, heavy, dtype=jnp.bfloat16):
    values = spread * jax.random.normal(own_key, shape, jnp.float32)
    if cuts:
        values = values * shard_levels(own_key, shape, cuts, -0.22, 0.18)
    return jnp.clip(spiked(values, jax.random.fold_in(own_key, 3), *heavy), -limit, limit).astype(dtype)


def setup_inputs(seed: int = 0) -> dict:
    streams_of = jax.random.split(jax.random.key(seed), 9)
    return {
        "queries": draw_queries(jax.random.fold_in(streams_of[8], 71), 0),
        "keys": draw_keys(jax.random.fold_in(streams_of[8], 71), 0),
        "values": scatter_about(streams_of[2], (SEQ, KV_HEADS * HDIM), 1.0, 6.0, ((0, 8), (1, 4))),
        "log_gate": draw_log_gate(jax.random.fold_in(streams_of[8], 71), 0),
        "log_sum": draw_log_sum(jax.random.fold_in(streams_of[8], 71), 0),
        "output": scatter_about(streams_of[5], (SEQ, HEADS * HDIM), 1.0, 6.0, ((0, 8), (1, 4))),
        "cotangent": scatter_about(streams_of[6], (SEQ, HEADS * HDIM), 2.0, 12.0, ((0, 8), (1, 4))),
        "normed": noise_with(streams_of[7], (SEQ, D), 1.0, 8.0, ((0, 8), (1, 4)), (0, 1, 8, 2.0)),
    }


NEG_LARGE = -1e30


def to_low(array):
    rounded = lax.optimization_barrier(array.astype(jnp.bfloat16))
    return rounded.astype(jnp.float32)


def reference(queries, keys, values, log_gate, log_sum, output, cotangent, normed):
    group_size = HEADS // KV_HEADS
    block_count = SEQ // TOK_DEV
    inverse_root = HDIM ** -0.5
    cumulative = jnp.cumsum(log_gate, axis=1)
    row_terms = jnp.sum((output.astype(jnp.float32) * cotangent.astype(jnp.float32)).reshape(SEQ, HEADS, HDIM), axis=2).T

    def by_group(array):
        return jnp.transpose(array.reshape(block_count, TOK_DEV, KV_HEADS, group_size, HDIM), (2, 0, 1, 3, 4))

    def rows_group(array):
        return jnp.transpose(array.reshape(KV_HEADS, group_size, block_count, TOK_DEV), (0, 2, 1, 3))

    query_blocks = by_group(queries)
    cotan_blocks = by_group(cotangent)
    cum_blocks = rows_group(cumulative)
    lse_blocks = rows_group(log_sum)
    term_blocks = rows_group(row_terms)
    key_heads = jnp.transpose(keys.reshape(SEQ, KV_HEADS, HDIM), (1, 0, 2))
    value_heads = jnp.transpose(values.reshape(SEQ, KV_HEADS, HDIM), (1, 0, 2))
    cum_keys = cumulative.reshape(KV_HEADS, group_size, SEQ)
    key_positions = jnp.arange(SEQ)

    def one_group(inputs):
        query_group, cotan_group, cum_group, lse_group, term_group, key_group, value_group, key_cum = inputs
        key_float = key_group.astype(jnp.float32)
        value_float = value_group.astype(jnp.float32)

        def one_block(state_now, pieces):
            key_total, value_total = state_now
            query_block, cotan_block, cum_block, lse_block, term_block, block_index = pieces
            query_positions = block_index * TOK_DEV + jnp.arange(TOK_DEV)
            query_float = query_block.astype(jnp.float32)
            cotan_float = cotan_block.astype(jnp.float32)
            scores = jnp.einsum("qgd,kd->gqk", query_float, key_float) * inverse_root
            scores = scores + cum_block[:, :, None] - key_cum[:, None, :] - lse_block[:, :, None]
            allowed = key_positions[None, :] <= query_positions[:, None]
            weights = jnp.exp(jnp.where(allowed[None], scores, NEG_LARGE))
            upstream = jnp.einsum("qgd,kd->gqk", cotan_float, value_float)
            dscore = weights * (upstream - term_block[:, :, None])
            weights_low = to_low(weights)
            dscore_low = to_low(dscore)
            query_part = jnp.einsum("gqk,kd->qgd", dscore_low, key_float) * inverse_root
            key_total = key_total + jnp.einsum("gqk,qgd->kd", dscore_low, query_float) * inverse_root
            value_total = value_total + jnp.einsum("gqk,qgd->kd", weights_low, cotan_float)
            return (key_total, value_total), query_part

        zeros_start = jnp.zeros((SEQ, HDIM), jnp.float32)
        totals, query_parts = lax.scan(one_block, (zeros_start, zeros_start),
                                       (query_group, cotan_group, cum_group, lse_group, term_group,
                                        jnp.arange(block_count)))
        return query_parts, totals[0], totals[1]

    query_parts, key_parts, value_parts = lax.map(one_group, (query_blocks, cotan_blocks, cum_blocks, lse_blocks,
                                                              term_blocks, key_heads, value_heads, cum_keys))
    query_grad = jnp.transpose(query_parts, (1, 2, 0, 3, 4)).reshape(SEQ, HEADS * HDIM).astype(jnp.bfloat16)
    key_grad = jnp.transpose(key_parts, (1, 0, 2)).reshape(SEQ, KV_HEADS * HDIM).astype(jnp.bfloat16)
    value_grad = jnp.transpose(value_parts, (1, 0, 2)).reshape(SEQ, KV_HEADS * HDIM).astype(jnp.bfloat16)
    weight_grad = jnp.dot(normed.T, key_grad, preferred_element_type=jnp.float32)
    return (query_grad, key_grad, value_grad, weight_grad)
```

```python
import functools

import jax
import jax.numpy as jnp
from jax import lax
from jax.experimental import pallas as pl
from jax.experimental.pallas import tpu as pltpu
from jax.sharding import PartitionSpec as P

HDIM = 64


NEG_LARGE = -1e30


def prefix(x, axis, combine, identity):
    size, place = (lax.axis_size(axis), lax.axis_index(axis))
    everything = lax.all_gather(x, axis)
    start = jnp.broadcast_to(jnp.asarray(identity, x.dtype), x.shape)

    def hop(k, before):
        reached = k < place
        new = combine(before, everything[k])
        return jnp.where(reached, new, before)

    return lax.fori_loop(0, size, hop, start)


def shifted(x, axis, by):
    size = lax.axis_size(axis)
    pairs = [(i, i + by) for i in range(size) if 0 <= i + by < size]
    return lax.ppermute(x, axis, pairs)


def shifted_2(x, axis, by):
    size = lax.axis_size(axis)
    return lax.ppermute(x, axis, [(i, (i + by) % size) for i in range(size)])


def add_pair(earlier, later):
    return earlier + later


def body(queries, keys, values, log_gate, log_sum, output, cotangent, normed):
    tokens = queries.shape[0]
    head_count = log_gate.shape[0]
    kv_width = keys.shape[1]
    kv_heads = kv_width // HDIM
    groups = head_count // kv_heads
    inverse_root = HDIM ** (-0.5)
    devices = lax.axis_size("sp")
    my_index = lax.axis_index("sp")
    depth = 8
    totals = jnp.sum(log_gate, axis=1)
    before = prefix(totals, "sp", add_pair, jnp.zeros_like(totals))
    cumulative = jnp.cumsum(log_gate, axis=1) + before[:, None]
    row_terms = jnp.sum(
        (output.astype(jnp.float32) * cotangent.astype(jnp.float32)).reshape(
            tokens, head_count, HDIM
        ),
        axis=2,
    ).T
    query_split = queries.reshape(tokens, kv_heads, groups, HDIM)
    cotan_split = cotangent.reshape(tokens, kv_heads, groups, HDIM)
    cum_rows = cumulative.reshape(kv_heads, groups, tokens)
    lse_rows = log_sum.reshape(kv_heads, groups, tokens)
    term_rows = row_terms.reshape(kv_heads, groups, tokens)
    positions = my_index * tokens + jnp.arange(tokens)
    last_row = my_index * tokens + tokens - 1

    def visit_bundle(bundle, bundle_cum, key_pos):
        count = bundle.shape[0]
        block_rows = bundle.shape[1]
        key_rows = count * block_rows
        flat = bundle.reshape(key_rows, 2 * kv_width)
        flat_cum = jnp.transpose(bundle_cum, (1, 0, 2)).reshape(kv_heads, groups, key_rows)
        flat_pos = key_pos.reshape(key_rows)
        key_part = flat[:, :kv_width].reshape(key_rows, kv_heads, HDIM)
        value_part = flat[:, kv_width:].reshape(key_rows, kv_heads, HDIM)

        def attend(unused):
            scores = (
                jnp.einsum(
                    "qhgd,khd->hgqk", query_split, key_part, preferred_element_type=jnp.float32
                )
                * inverse_root
            )
            scores = (
                scores + cum_rows[:, :, :, None] - flat_cum[:, :, None, :] - lse_rows[:, :, :, None]
            )
            allowed = flat_pos[None, :] <= positions[:, None]
            weights = jnp.exp(jnp.where(allowed, scores, NEG_LARGE))
            upstream = jnp.einsum(
                "qhgd,khd->hgqk", cotan_split, value_part, preferred_element_type=jnp.float32
            )
            dscore_low = (weights * (upstream - term_rows[:, :, :, None])).astype(jnp.bfloat16)
            weights_low = weights.astype(jnp.bfloat16)
            query_add = (
                jnp.einsum(
                    "hgqk,khd->qhgd", dscore_low, key_part, preferred_element_type=jnp.float32
                )
                * inverse_root
            )
            key_add = (
                jnp.einsum(
                    "hgqk,qhgd->khd", dscore_low, query_split, preferred_element_type=jnp.float32
                )
                * inverse_root
            )
            value_add = jnp.einsum(
                "hgqk,qhgd->khd", weights_low, cotan_split, preferred_element_type=jnp.float32
            )
            joined = jnp.concatenate(
                [key_add.reshape(key_rows, kv_width), value_add.reshape(key_rows, kv_width)], axis=1
            )
            return (query_add, joined.reshape(count, block_rows, 2 * kv_width))

        def nothing(unused):
            return (
                jnp.zeros((tokens, kv_heads, groups, HDIM), jnp.float32),
                jnp.zeros((count, block_rows, 2 * kv_width), jnp.float32),
            )

        return lax.cond(jnp.min(flat_pos) <= last_row, attend, nothing, 0)

    stacked = jnp.concatenate([keys, values], axis=1)
    query_start = jnp.zeros((tokens, kv_heads, groups, HDIM), jnp.float32)
    copies = jnp.arange(depth)
    turns = devices // depth
    bundle_pieces = [stacked]
    bundle_cums = [cumulative]
    for step in range(1, depth):
        bundle_pieces.append(shifted(stacked, "sp", step))
        bundle_cums.append(shifted(cumulative, "sp", step))

    def turn(turn_index, state_now):
        query_total, bundle, bundle_cum, bundle_grads = state_now
        anchor = (my_index - depth * turn_index) % devices
        blocks = (anchor - copies) % devices
        key_pos = blocks[:, None] * tokens + jnp.arange(tokens)[None, :]
        query_add, grad_add = visit_bundle(bundle, bundle_cum, key_pos)
        bundle = shifted(bundle, "sp", depth)
        bundle_cum, bundle_grads = shifted_2((bundle_cum, bundle_grads + grad_add), "sp", depth)
        return (query_total + query_add, bundle, bundle_cum, bundle_grads)

    start_state = (
        query_start,
        jnp.stack(bundle_pieces),
        jnp.stack(bundle_cums),
        jnp.zeros((depth, tokens, 2 * kv_width), jnp.float32),
    )
    finished = lax.fori_loop(0, turns, turn, start_state)
    query_total = finished[0]
    final_grads = finished[3]
    gradients = final_grads[0]
    for step in range(1, depth):
        gradients = gradients + shifted(final_grads[step], "sp", -step)
    query_grad = query_total.reshape(tokens, head_count * HDIM).astype(jnp.bfloat16)
    key_grad = gradients[:, :kv_width].astype(jnp.bfloat16)
    value_grad = gradients[:, kv_width:].astype(jnp.bfloat16)
    whole_rows = lax.all_gather(normed, "tp", axis=1, tiled=True)
    weight_grad = lax.psum_scatter(
        lax.dot_general(
            whole_rows, key_grad, (((0,), (0,)), ((), ())), preferred_element_type=jnp.float32
        ),
        "sp",
        scatter_dimension=0,
        tiled=True,
    )
    return (query_grad, key_grad, value_grad, weight_grad)


F32, BF16 = (jnp.float32, jnp.bfloat16)
HBM = pl.BlockSpec(memory_space=pl.ANY)
NT = (((1,), (1,)), ((), ()))
NN = (((1,), (0,)), ((), ()))


def dot(a, b, dims=NN, precision=None):
    return lax.dot_general(a, b, dims, precision=precision, preferred_element_type=F32)


def fused(
    n, m,
    q_hbm, k_hbm, v_hbm, gate_hbm, lse_hbm, out_hbm, cot_hbm, normed_hbm,
    qg_ref, kg_ref, vg_ref, wg_ref,
    q_in, k_in, v_in, gate_in, lse_in, out_in, cot_in,
    normed_all, kv, gates, diag, dq, grad_send, grad_recv, grad_own, w_send, w_recv, w_own,
    in_sem, norm_in_sem, norm_send, norm_recv, kv_send, kv_recv, gate_send, gate_recv,
    gr_send, gr_recv, wt_send, wt_recv,
):
    me = lax.axis_index("sp")
    tp = lax.axis_index("tp")
    tokens, width = q_in.shape
    groups = gate_in.shape[0]
    span = groups * tokens
    chunk = normed_all.shape[2]
    per = normed_all.shape[0] // m
    scale = HDIM ** (-0.5)

    barrier = pltpu.get_barrier_semaphore()
    for k in range(1, n):
        pl.semaphore_signal(barrier, inc=1, device_id={"sp": lax.rem(me + k, n)}, device_id_type=pl.DeviceIdType.MESH)
    for k in range(1, m):
        pl.semaphore_signal(barrier, inc=1, device_id={"tp": lax.rem(tp + k, m)}, device_id_type=pl.DeviceIdType.MESH)

    pairs = [
        (k_hbm, k_in), (v_hbm, v_in), (gate_hbm, gate_in), (q_hbm, q_in), (cot_hbm, cot_in),
        (out_hbm, out_in), (lse_hbm, lse_in),
    ]
    loads = [pltpu.make_async_copy(a, b, in_sem.at[i]) for i, (a, b) in enumerate(pairs)]
    for load in loads:
        load.start()
    norm_loads = [
        pltpu.make_async_copy(
            normed_hbm.at[:, pl.ds(c * chunk, chunk)], normed_all.at[tp * per + c], norm_in_sem.at[c]
        )
        for c in range(per)
    ]
    for load in norm_loads:
        load.start()

    for load in loads[:3]:
        load.wait()
    kv[0] = jnp.concatenate([k_in[...], v_in[...]], axis=1)
    rows = lax.broadcasted_iota(jnp.int32, (tokens, tokens), 0)
    cols = lax.broadcasted_iota(jnp.int32, (tokens, tokens), 1)
    gate = gate_in[...]
    local = dot(gate, (rows <= cols).astype(F32), NN, lax.Precision.HIGHEST)
    total = jnp.broadcast_to(jnp.sum(gate, axis=1, keepdims=True), gate.shape)
    gates[0, 0:groups, :] = total - local
    gates[0, groups:, :] = total

    for load in norm_loads:
        load.wait()
    pl.semaphore_wait(barrier, n - 1 + m - 1)

    def kv_copy(k):
        where = {"sp": lax.rem(me + k, n)}
        return (
            pltpu.make_async_remote_copy(gates.at[0], gates.at[k], gate_send.at[k], gate_recv.at[k], where, pl.DeviceIdType.MESH),
            pltpu.make_async_remote_copy(kv.at[0], kv.at[k], kv_send.at[k], kv_recv.at[k], where, pl.DeviceIdType.MESH),
        )

    def norm_copy(k):
        mine = normed_all.at[pl.ds(tp * per, per)]
        return pltpu.make_async_remote_copy(
            mine, mine, norm_send.at[k], norm_recv.at[k], {"tp": lax.rem(tp + k, m)}, pl.DeviceIdType.MESH
        )

    def norm_arrival(k):
        theirs = normed_all.at[pl.ds(lax.rem(tp + m - k, m) * per, per)]
        return pltpu.make_async_remote_copy(
            theirs, theirs, norm_send.at[k], norm_recv.at[k], {"tp": lax.rem(tp + k, m)}, pl.DeviceIdType.MESH
        )

    def grad_copy(k):
        where = {"sp": lax.rem(me + n - k, n)}
        return pltpu.make_async_remote_copy(
            grad_send.at[k], grad_recv.at[k], gr_send.at[k], gr_recv.at[k], where, pl.DeviceIdType.MESH
        )

    def weight_copy(k):
        where = {"sp": lax.rem(me + k, n)}
        return pltpu.make_async_remote_copy(
            w_send.at[k], w_recv.at[k], wt_send.at[k], wt_recv.at[k], where, pl.DeviceIdType.MESH
        )

    for k in range(1, n):
        @pl.when(me + k < n)
        def _(k=k):
            for copy in kv_copy(k):
                copy.start()
    for k in range(1, m):
        norm_copy(k).start()

    for load in loads[3:]:
        load.wait()
    low = lax.broadcasted_iota(jnp.int32, (tokens, 2 * HDIM), 1) < HDIM
    for pair in range(groups // 2):
        lanes = pl.ds(2 * HDIM * pair, 2 * HDIM)
        two = q_in[:, lanes].astype(F32) * scale
        up = cot_in[:, lanes].astype(F32)
        for half in range(2):
            head = 2 * pair + half
            q_head = two if half == 0 else pltpu.roll(two, HDIM, 1)
            c_head = up if half == 1 else pltpu.roll(up, HDIM, 1)
            diag[pl.ds(head * tokens, tokens), :] = jnp.where(low, q_head, 0.0).astype(BF16)
            diag[pl.ds(span + head * tokens, tokens), :] = jnp.where(low, 0.0, c_head).astype(BF16)
    product = out_in[...].astype(F32) * cot_in[...].astype(F32)
    delta = jnp.sum(product.T.reshape(groups, HDIM, tokens), axis=1)
    row_term = local - lse_in[...]

    def visit(k, key_rows):
        block = kv[k]
        both = dot(block, diag[...], NT)
        key_cols = key_rows.T
        prob_parts, score_parts = ([], [])
        for h in range(groups):
            score = both[:, h * tokens : (h + 1) * tokens] + (row_term[h : h + 1, :] + key_cols[:, h : h + 1])
            if k == 0:
                score = jnp.where(rows <= cols, score, NEG_LARGE)
            prob = jnp.exp(score)
            dprob = both[:, span + h * tokens : span + (h + 1) * tokens]
            prob_parts.append(prob.astype(BF16))
            score_parts.append((prob * (dprob - delta[h : h + 1, :])).astype(BF16))
        dscore = jnp.concatenate(score_parts, axis=1)
        weights = jnp.concatenate(score_parts + prob_parts, axis=1)
        grads = dot(weights, diag[...])
        key_t = block.T[:HDIM, :]
        dq_add = dot(key_t, dscore)
        if k == 0:
            dq[...] = dq_add
            grad_own[...] = grads
        else:
            dq[...] += dq_add
            grad_send[k] = grads.astype(BF16)

    visit(0, jnp.concatenate([-local, -local], axis=0))

    for k in range(1, n):
        @pl.when(k <= me)
        def _(k=k):
            for copy in kv_copy(k):
                copy.wait_recv()
            key_rows = gates[k, 0:groups, :]
            for between in range(1, k):
                key_rows = key_rows + gates[between, groups:, :]
            visit(k, jnp.concatenate([key_rows, key_rows], axis=0))
            grad_copy(k).start()

    for pair in range(groups // 2):
        first = dq[:, pl.ds(2 * pair * tokens, tokens)]
        second = dq[:, pl.ds((2 * pair + 1) * tokens, tokens)]
        joined = jnp.concatenate([first, second], axis=0) * scale
        qg_ref[:, pl.ds(2 * HDIM * pair, 2 * HDIM)] = joined.T.astype(BF16)

    for k in range(1, n):
        @pl.when(me + k < n)
        def _(k=k):
            grad_copy(k).wait_recv()
            grad_own[...] += grad_recv[k].astype(F32)
    grads = grad_own[...]
    kg_ref[...] = grads[:, :HDIM].astype(BF16)
    vg_ref[...] = grads[:, HDIM:].astype(BF16)
    key_grad_t = grads.T[:HDIM, :].astype(BF16)

    for k in range(1, m):
        norm_arrival(k).wait_recv()
    for k in range(1, n):
        w_send[k] = dot(key_grad_t, normed_all[lax.rem(me + k, n)]).astype(BF16)
        weight_copy(k).start()
    w_own[...] = dot(key_grad_t, normed_all[me])
    for k in range(1, n):
        weight_copy(k).wait_recv()
        w_own[...] += w_recv[k].astype(F32)
    wg_ref[...] = w_own[...].T

    for k in range(1, m):
        norm_copy(k).wait_send()
    for k in range(1, n):
        weight_copy(k).wait_send()

        @pl.when(me + k < n)
        def _(k=k):
            for copy in kv_copy(k):
                copy.wait_send()

        @pl.when(k <= me)
        def _(k=k):
            grad_copy(k).wait_send()


def one_kernel(n, m, queries, keys, values, log_gate, log_sum, output, cotangent, normed):
    tokens, width = queries.shape
    kv_width = keys.shape[1]
    groups = log_gate.shape[0]
    per = n // m
    chunk = normed.shape[1] // per
    pair = 2 * HDIM
    vmem = pltpu.VMEM
    dma = pltpu.SemaphoreType.DMA
    full = pl.BlockSpec(memory_space=pltpu.VMEM)
    return tuple(
        pl.pallas_call(
            functools.partial(fused, n, m),
            out_shape=(
                jax.ShapeDtypeStruct((tokens, width), BF16),
                jax.ShapeDtypeStruct((tokens, kv_width), BF16),
                jax.ShapeDtypeStruct((tokens, kv_width), BF16),
                jax.ShapeDtypeStruct((chunk, kv_width), F32),
            ),
            in_specs=[HBM] * 8,
            out_specs=(full,) * 4,
            scratch_shapes=[
                vmem((tokens, width), BF16), vmem((tokens, kv_width), BF16), vmem((tokens, kv_width), BF16),
                vmem((groups, tokens), F32), vmem((groups, tokens), F32),
                vmem((tokens, width), BF16), vmem((tokens, width), BF16),
                vmem((n, tokens, chunk), BF16), vmem((n, tokens, pair), BF16), vmem((n, 2 * groups, tokens), F32),
                vmem((2 * groups * tokens, pair), BF16), vmem((HDIM, groups * tokens), F32),
                vmem((n, tokens, pair), BF16), vmem((n, tokens, pair), BF16), vmem((tokens, pair), F32),
                vmem((n, HDIM, chunk), BF16), vmem((n, HDIM, chunk), BF16), vmem((HDIM, chunk), F32),
                dma((7,)), dma((per,)), dma((m,)), dma((m,)), dma((n,)), dma((n,)), dma((n,)), dma((n,)),
                dma((n,)), dma((n,)), dma((n,)), dma((n,)),
            ],
            compiler_params=pltpu.CompilerParams(collective_id=0, has_side_effects=True),
        )(queries, keys, values, log_gate, log_sum, output, cotangent, normed)
    )


def chosen(n, m, *arrays):
    queries, keys, log_gate, normed = (arrays[0], arrays[1], arrays[3], arrays[7])
    whole = (
        n % m == 0
        and keys.shape[1] == HDIM
        and log_gate.shape[0] == 4
        and queries.shape[0] == 128
        and normed.shape[1] % (n // m * 128) == 0
    )
    return one_kernel(n, m, *arrays) if whole else body(*arrays)


def solution(mesh):
    n_sp, n_tp = mesh.shape["sp"], mesh.shape["tp"]
    in_specs = (
        P("sp", "tp"),
        P("sp", "tp"),
        P("sp", "tp"),
        P("tp", "sp"),
        P("tp", "sp"),
        P("sp", "tp"),
        P("sp", "tp"),
        P("sp", "tp"),
    )
    out_specs = (P("sp", "tp"), P("sp", "tp"), P("sp", "tp"), P("sp", "tp"))
    return jax.shard_map(functools.partial(chosen, n_sp, n_tp), mesh=mesh, in_specs=in_specs, out_specs=out_specs, check_vma=False)
```

```python
import functools

import jax
import jax.numpy as jnp
from jax import lax
from jax.experimental import pallas as pl
from jax.experimental.pallas import tpu as pltpu
from jax.sharding import PartitionSpec as P

HDIM = 64


NEG_LARGE = -1e30


def prefix(x, axis, combine, identity):
    size, place = (lax.axis_size(axis), lax.axis_index(axis))
    everything = lax.all_gather(x, axis)
    start = jnp.broadcast_to(jnp.asarray(identity, x.dtype), x.shape)

    def hop(k, before):
        reached = k < place
        new = combine(before, everything[k])
        return jnp.where(reached, new, before)

    return lax.fori_loop(0, size, hop, start)


def shifted(x, axis, by):
    size = lax.axis_size(axis)
    pairs = [(i, i + by) for i in range(size) if 0 <= i + by < size]
    return lax.ppermute(x, axis, pairs)


def shifted_2(x, axis, by):
    size = lax.axis_size(axis)
    return lax.ppermute(x, axis, [(i, (i + by) % size) for i in range(size)])


def add_pair(earlier, later):
    return earlier + later


def body(queries, keys, values, log_gate, log_sum, output, cotangent, normed):
    tokens = queries.shape[0]
    head_count = log_gate.shape[0]
    kv_width = keys.shape[1]
    kv_heads = kv_width // HDIM
    groups = head_count // kv_heads
    inverse_root = HDIM ** (-0.5)
    devices = lax.axis_size("sp")
    my_index = lax.axis_index("sp")
    depth = 8
    totals = jnp.sum(log_gate, axis=1)
    before = prefix(totals, "sp", add_pair, jnp.zeros_like(totals))
    cumulative = jnp.cumsum(log_gate, axis=1) + before[:, None]
    row_terms = jnp.sum(
        (output.astype(jnp.float32) * cotangent.astype(jnp.float32)).reshape(
            tokens, head_count, HDIM
        ),
        axis=2,
    ).T
    query_split = queries.reshape(tokens, kv_heads, groups, HDIM)
    cotan_split = cotangent.reshape(tokens, kv_heads, groups, HDIM)
    cum_rows = cumulative.reshape(kv_heads, groups, tokens)
    lse_rows = log_sum.reshape(kv_heads, groups, tokens)
    term_rows = row_terms.reshape(kv_heads, groups, tokens)
    positions = my_index * tokens + jnp.arange(tokens)
    last_row = my_index * tokens + tokens - 1

    def visit_bundle(bundle, bundle_cum, key_pos):
        count = bundle.shape[0]
        block_rows = bundle.shape[1]
        key_rows = count * block_rows
        flat = bundle.reshape(key_rows, 2 * kv_width)
        flat_cum = jnp.transpose(bundle_cum, (1, 0, 2)).reshape(kv_heads, groups, key_rows)
        flat_pos = key_pos.reshape(key_rows)
        key_part = flat[:, :kv_width].reshape(key_rows, kv_heads, HDIM)
        value_part = flat[:, kv_width:].reshape(key_rows, kv_heads, HDIM)

        def attend(unused):
            scores = (
                jnp.einsum(
                    "qhgd,khd->hgqk", query_split, key_part, preferred_element_type=jnp.float32
                )
                * inverse_root
            )
            scores = (
                scores + cum_rows[:, :, :, None] - flat_cum[:, :, None, :] - lse_rows[:, :, :, None]
            )
            allowed = flat_pos[None, :] <= positions[:, None]
            weights = jnp.exp(jnp.where(allowed, scores, NEG_LARGE))
            upstream = jnp.einsum(
                "qhgd,khd->hgqk", cotan_split, value_part, preferred_element_type=jnp.float32
            )
            dscore_low = (weights * (upstream - term_rows[:, :, :, None])).astype(jnp.bfloat16)
            weights_low = weights.astype(jnp.bfloat16)
            query_add = (
                jnp.einsum(
                    "hgqk,khd->qhgd", dscore_low, key_part, preferred_element_type=jnp.float32
                )
                * inverse_root
            )
            key_add = (
                jnp.einsum(
                    "hgqk,qhgd->khd", dscore_low, query_split, preferred_element_type=jnp.float32
                )
                * inverse_root
            )
            value_add = jnp.einsum(
                "hgqk,qhgd->khd", weights_low, cotan_split, preferred_element_type=jnp.float32
            )
            joined = jnp.concatenate(
                [key_add.reshape(key_rows, kv_width), value_add.reshape(key_rows, kv_width)], axis=1
            )
            return (query_add, joined.reshape(count, block_rows, 2 * kv_width))

        def nothing(unused):
            return (
                jnp.zeros((tokens, kv_heads, groups, HDIM), jnp.float32),
                jnp.zeros((count, block_rows, 2 * kv_width), jnp.float32),
            )

        return lax.cond(jnp.min(flat_pos) <= last_row, attend, nothing, 0)

    stacked = jnp.concatenate([keys, values], axis=1)
    query_start = jnp.zeros((tokens, kv_heads, groups, HDIM), jnp.float32)
    copies = jnp.arange(depth)
    turns = devices // depth
    bundle_pieces = [stacked]
    bundle_cums = [cumulative]
    for step in range(1, depth):
        bundle_pieces.append(shifted(stacked, "sp", step))
        bundle_cums.append(shifted(cumulative, "sp", step))

    def turn(turn_index, state_now):
        query_total, bundle, bundle_cum, bundle_grads = state_now
        anchor = (my_index - depth * turn_index) % devices
        blocks = (anchor - copies) % devices
        key_pos = blocks[:, None] * tokens + jnp.arange(tokens)[None, :]
        query_add, grad_add = visit_bundle(bundle, bundle_cum, key_pos)
        bundle = shifted(bundle, "sp", depth)
        bundle_cum, bundle_grads = shifted_2((bundle_cum, bundle_grads + grad_add), "sp", depth)
        return (query_total + query_add, bundle, bundle_cum, bundle_grads)

    start_state = (
        query_start,
        jnp.stack(bundle_pieces),
        jnp.stack(bundle_cums),
        jnp.zeros((depth, tokens, 2 * kv_width), jnp.float32),
    )
    finished = lax.fori_loop(0, turns, turn, start_state)
    query_total = finished[0]
    final_grads = finished[3]
    gradients = final_grads[0]
    for step in range(1, depth):
        gradients = gradients + shifted(final_grads[step], "sp", -step)
    query_grad = query_total.reshape(tokens, head_count * HDIM).astype(jnp.bfloat16)
    key_grad = gradients[:, :kv_width].astype(jnp.bfloat16)
    value_grad = gradients[:, kv_width:].astype(jnp.bfloat16)
    whole_rows = lax.all_gather(normed, "tp", axis=1, tiled=True)
    weight_grad = lax.psum_scatter(
        lax.dot_general(
            whole_rows, key_grad, (((0,), (0,)), ((), ())), preferred_element_type=jnp.float32
        ),
        "sp",
        scatter_dimension=0,
        tiled=True,
    )
    return (query_grad, key_grad, value_grad, weight_grad)


F32, BF16 = (jnp.float32, jnp.bfloat16)
HBM = pl.BlockSpec(memory_space=pl.ANY)
NT = (((1,), (1,)), ((), ()))
NN = (((1,), (0,)), ((), ()))


def dot(a, b, dims=NN, precision=None):
    return lax.dot_general(a, b, dims, precision=precision, preferred_element_type=F32)


def fused(
    n, m,
    q_hbm, k_hbm, v_hbm, gate_hbm, lse_hbm, out_hbm, cot_hbm, normed_hbm,
    qg_ref, kg_ref, vg_ref, wg_ref,
    q_in, gate_in, lse_in, out_in, cot_in,
    normed_all, kv, gates, diag, dq, grad_send, grad_recv, grad_own, w_send, w_recv,
    in_sem, norm_in_sem, norm_send, norm_recv, kv_send, kv_recv, gate_send, gate_recv,
    gr_send, gr_recv, wt_send, wt_recv,
):
    me = lax.axis_index("sp")
    tp = lax.axis_index("tp")
    tokens, width = q_in.shape
    groups = gate_in.shape[0]
    span = groups * tokens
    chunk = normed_all.shape[2]
    per = normed_all.shape[0] // m
    scale = HDIM ** (-0.5)

    barrier = pltpu.get_barrier_semaphore()
    for k in range(1, n):
        pl.semaphore_signal(barrier, inc=1, device_id={"sp": lax.rem(me + k, n)}, device_id_type=pl.DeviceIdType.MESH)
    for k in range(1, m):
        pl.semaphore_signal(barrier, inc=1, device_id={"tp": lax.rem(tp + k, m)}, device_id_type=pl.DeviceIdType.MESH)

    pairs = [
        (k_hbm, kv.at[0, pl.ds(0, HDIM)]), (v_hbm, kv.at[0, pl.ds(HDIM, HDIM)]), (gate_hbm, gate_in), (q_hbm, q_in), (cot_hbm, cot_in),
        (out_hbm, out_in), (lse_hbm, lse_in),
    ]
    loads = [pltpu.make_async_copy(a, b, in_sem.at[i]) for i, (a, b) in enumerate(pairs)]
    for load in loads:
        load.start()
    norm_loads = [
        pltpu.make_async_copy(
            normed_hbm.at[:, pl.ds(c * chunk, chunk)], normed_all.at[tp * per + c], norm_in_sem.at[c]
        )
        for c in range(per)
    ]
    for load in norm_loads:
        load.start()

    for load in loads[:3]:
        load.wait()
    rows = lax.broadcasted_iota(jnp.int32, (tokens, tokens), 0)
    cols = lax.broadcasted_iota(jnp.int32, (tokens, tokens), 1)
    gate = gate_in[...]
    local = dot(gate, (rows <= cols).astype(F32), NN, lax.Precision.HIGHEST)
    total = jnp.broadcast_to(jnp.sum(gate, axis=1, keepdims=True), gate.shape)
    gates[0, 0:groups, :] = total - local
    gates[0, groups:, :] = total

    for load in norm_loads:
        load.wait()
    pl.semaphore_wait(barrier, n - 1 + m - 1)

    def kv_copy(k):
        where = {"sp": lax.rem(me + k, n)}
        return (
            pltpu.make_async_remote_copy(gates.at[0], gates.at[k], gate_send.at[k], gate_recv.at[k], where, pl.DeviceIdType.MESH),
            pltpu.make_async_remote_copy(kv.at[0], kv.at[k], kv_send.at[k], kv_recv.at[k], where, pl.DeviceIdType.MESH),
        )

    def norm_copy(k):
        mine = normed_all.at[pl.ds(tp * per, per)]
        return pltpu.make_async_remote_copy(
            mine, mine, norm_send.at[k], norm_recv.at[k], {"tp": lax.rem(tp + k, m)}, pl.DeviceIdType.MESH
        )

    def norm_arrival(k):
        theirs = normed_all.at[pl.ds(lax.rem(tp + m - k, m) * per, per)]
        return pltpu.make_async_remote_copy(
            theirs, theirs, norm_send.at[k], norm_recv.at[k], {"tp": lax.rem(tp + k, m)}, pl.DeviceIdType.MESH
        )

    def grad_copy(k):
        where = {"sp": lax.rem(me + n - k, n)}
        return pltpu.make_async_remote_copy(
            grad_send.at[k], grad_recv.at[k], gr_send.at[k], gr_recv.at[k], where, pl.DeviceIdType.MESH
        )

    def weight_copy(k):
        where = {"sp": lax.rem(me + k, n)}
        return pltpu.make_async_remote_copy(
            w_send.at[k], w_recv.at[k], wt_send.at[k], wt_recv.at[k], where, pl.DeviceIdType.MESH
        )

    for k in range(1, n):
        @pl.when(me + k < n)
        def _(k=k):
            for copy in kv_copy(k):
                copy.start()
    for k in range(1, m):
        norm_copy(k).start()

    for load in loads[3:]:
        load.wait()
    low = lax.broadcasted_iota(jnp.int32, (tokens, 2 * HDIM), 1) < HDIM
    for pair in range(groups // 2):
        lanes = pl.ds(2 * HDIM * pair, 2 * HDIM)
        two = q_in[:, lanes].astype(F32) * scale
        up = cot_in[:, lanes].astype(F32)
        for half in range(2):
            head = 2 * pair + half
            q_head = two if half == 0 else pltpu.roll(two, HDIM, 1)
            c_head = up if half == 1 else pltpu.roll(up, HDIM, 1)
            diag[pl.ds(head * tokens, tokens), :] = jnp.where(low, q_head, 0.0).astype(BF16)
            diag[pl.ds(span + head * tokens, tokens), :] = jnp.where(low, 0.0, c_head).astype(BF16)
    product = out_in[...].astype(F32) * cot_in[...].astype(F32)
    delta = jnp.sum(product.T.reshape(groups, HDIM, tokens), axis=1)
    row_term = local - lse_in[...]

    def visit(k, key_rows):
        block = kv[k]
        both = dot(block.T, diag[...], NT)
        key_cols = key_rows.T
        prob_parts, score_parts = ([], [])
        for h in range(groups):
            score = both[:, h * tokens : (h + 1) * tokens] + (row_term[h : h + 1, :] + key_cols[:, h : h + 1])
            if k == 0:
                score = jnp.where(rows <= cols, score, NEG_LARGE)
            prob = jnp.exp(score)
            dprob = both[:, span + h * tokens : span + (h + 1) * tokens]
            prob_parts.append(prob.astype(BF16))
            score_parts.append((prob * (dprob - delta[h : h + 1, :])).astype(BF16))
        dscore = jnp.concatenate(score_parts, axis=1)
        weights = jnp.concatenate(score_parts + prob_parts, axis=1)
        grads = dot(weights, diag[...])
        dq_add = dot(block[:HDIM, :], dscore)
        if k == 0:
            dq[...] = dq_add
            grad_own[...] = grads
        else:
            dq[...] += dq_add
            grad_send[k] = grads.astype(BF16)

    visit(0, jnp.concatenate([-local, -local], axis=0))

    for k in range(1, n):
        @pl.when(k <= me)
        def _(k=k):
            for copy in kv_copy(k):
                copy.wait_recv()
            key_rows = gates[k, 0:groups, :]
            for between in range(1, k):
                key_rows = key_rows + gates[between, groups:, :]
            visit(k, jnp.concatenate([key_rows, key_rows], axis=0))
            grad_copy(k).start()

    for pair in range(groups // 2):
        first = dq[:, pl.ds(2 * pair * tokens, tokens)]
        second = dq[:, pl.ds((2 * pair + 1) * tokens, tokens)]
        joined = jnp.concatenate([first, second], axis=0) * scale
        qg_ref[:, pl.ds(2 * HDIM * pair, 2 * HDIM)] = joined.T.astype(BF16)

    for k in range(1, n):
        @pl.when(me + k < n)
        def _(k=k):
            grad_copy(k).wait_recv()
            grad_own[...] += grad_recv[k].astype(F32)
    grads = grad_own[...].T.astype(BF16)
    key_grad_t = grads[:HDIM, :]
    kg_ref[...] = key_grad_t
    vg_ref[...] = grads[HDIM:, :]

    for k in range(1, m):
        norm_arrival(k).wait_recv()
    for k in range(1, n):
        w_send[k] = dot(key_grad_t, normed_all[lax.rem(me + k, n)]).astype(BF16)
        weight_copy(k).start()
    wg_ref[...] = dot(key_grad_t, normed_all[me])
    for k in range(1, n):
        weight_copy(k).wait_recv()
        wg_ref[...] += w_recv[k].astype(F32)

    for k in range(1, m):
        norm_copy(k).wait_send()
    for k in range(1, n):
        weight_copy(k).wait_send()

        @pl.when(me + k < n)
        def _(k=k):
            for copy in kv_copy(k):
                copy.wait_send()

        @pl.when(k <= me)
        def _(k=k):
            grad_copy(k).wait_send()


def one_kernel(n, m, queries, keys, values, log_gate, log_sum, output, cotangent, normed):
    tokens, width = queries.shape
    kv_width = keys.shape[1]
    groups = log_gate.shape[0]
    per = n // m
    chunk = normed.shape[1] // per
    pair = 2 * HDIM
    vmem = pltpu.VMEM
    dma = pltpu.SemaphoreType.DMA
    full = pl.BlockSpec(memory_space=pltpu.VMEM)
    query_grad, key_grad, value_grad, weight_grad = pl.pallas_call(
            functools.partial(fused, n, m),
            out_shape=(
                jax.ShapeDtypeStruct((tokens, width), BF16),
                jax.ShapeDtypeStruct((kv_width, tokens), BF16),
                jax.ShapeDtypeStruct((kv_width, tokens), BF16),
                jax.ShapeDtypeStruct((kv_width, chunk), F32),
            ),
            in_specs=[HBM] * 8,
            out_specs=(full,) * 4,
            scratch_shapes=[
                vmem((tokens, width), BF16),
                vmem((groups, tokens), F32), vmem((groups, tokens), F32),
                vmem((tokens, width), BF16), vmem((tokens, width), BF16),
                vmem((n, tokens, chunk), BF16), vmem((n, tokens, pair), BF16), vmem((n, 2 * groups, tokens), F32),
                vmem((2 * groups * tokens, pair), BF16), vmem((HDIM, groups * tokens), F32),
                vmem((n, tokens, pair), BF16), vmem((n, tokens, pair), BF16), vmem((tokens, pair), F32),
                vmem((n, HDIM, chunk), BF16), vmem((n, HDIM, chunk), BF16),
                dma((7,)), dma((per,)), dma((m,)), dma((m,)), dma((n,)), dma((n,)), dma((n,)), dma((n,)),
                dma((n,)), dma((n,)), dma((n,)), dma((n,)),
            ],
            compiler_params=pltpu.CompilerParams(collective_id=0, has_side_effects=True),
        )(queries, keys.T, values.T, log_gate, log_sum, output, cotangent, normed)
    return (query_grad, key_grad.T, value_grad.T, weight_grad.T)


def chosen(n, m, *arrays):
    queries, keys, log_gate, normed = (arrays[0], arrays[1], arrays[3], arrays[7])
    whole = (
        n % m == 0
        and keys.shape[1] == HDIM
        and log_gate.shape[0] == 4
        and queries.shape[0] == 128
        and normed.shape[1] % (n // m * 128) == 0
    )
    return one_kernel(n, m, *arrays) if whole else body(*arrays)


def solution(mesh):
    n_sp, n_tp = mesh.shape["sp"], mesh.shape["tp"]
    in_specs = (
        P("sp", "tp"),
        P("sp", "tp"),
        P("sp", "tp"),
        P("tp", "sp"),
        P("tp", "sp"),
        P("sp", "tp"),
        P("sp", "tp"),
        P("sp", "tp"),
    )
    out_specs = (P("sp", "tp"), P("sp", "tp"), P("sp", "tp"), P("sp", "tp"))
    return jax.shard_map(functools.partial(chosen, n_sp, n_tp), mesh=mesh, in_specs=in_specs, out_specs=out_specs, check_vma=False)
```

```python
import functools

import jax
import jax.numpy as jnp
from jax import lax
from jax.experimental import pallas as pl
from jax.experimental.pallas import tpu as pltpu
from jax.sharding import PartitionSpec as P

HDIM = 64


NEG_LARGE = -1e30


def prefix(x, axis, combine, identity):
    size, place = (lax.axis_size(axis), lax.axis_index(axis))
    everything = lax.all_gather(x, axis)
    start = jnp.broadcast_to(jnp.asarray(identity, x.dtype), x.shape)

    def hop(k, before):
        reached = k < place
        new = combine(before, everything[k])
        return jnp.where(reached, new, before)

    return lax.fori_loop(0, size, hop, start)


def shifted(x, axis, by):
    size = lax.axis_size(axis)
    pairs = [(i, i + by) for i in range(size) if 0 <= i + by < size]
    return lax.ppermute(x, axis, pairs)


def shifted_2(x, axis, by):
    size = lax.axis_size(axis)
    return lax.ppermute(x, axis, [(i, (i + by) % size) for i in range(size)])


def add_pair(earlier, later):
    return earlier + later


def body(queries, keys, values, log_gate, log_sum, output, cotangent, normed):
    tokens = queries.shape[0]
    head_count = log_gate.shape[0]
    kv_width = keys.shape[1]
    kv_heads = kv_width // HDIM
    groups = head_count // kv_heads
    inverse_root = HDIM ** (-0.5)
    devices = lax.axis_size("sp")
    my_index = lax.axis_index("sp")
    depth = 8
    totals = jnp.sum(log_gate, axis=1)
    before = prefix(totals, "sp", add_pair, jnp.zeros_like(totals))
    cumulative = jnp.cumsum(log_gate, axis=1) + before[:, None]
    row_terms = jnp.sum(
        (output.astype(jnp.float32) * cotangent.astype(jnp.float32)).reshape(
            tokens, head_count, HDIM
        ),
        axis=2,
    ).T
    query_split = queries.reshape(tokens, kv_heads, groups, HDIM)
    cotan_split = cotangent.reshape(tokens, kv_heads, groups, HDIM)
    cum_rows = cumulative.reshape(kv_heads, groups, tokens)
    lse_rows = log_sum.reshape(kv_heads, groups, tokens)
    term_rows = row_terms.reshape(kv_heads, groups, tokens)
    positions = my_index * tokens + jnp.arange(tokens)
    last_row = my_index * tokens + tokens - 1

    def visit_bundle(bundle, bundle_cum, key_pos):
        count = bundle.shape[0]
        block_rows = bundle.shape[1]
        key_rows = count * block_rows
        flat = bundle.reshape(key_rows, 2 * kv_width)
        flat_cum = jnp.transpose(bundle_cum, (1, 0, 2)).reshape(kv_heads, groups, key_rows)
        flat_pos = key_pos.reshape(key_rows)
        key_part = flat[:, :kv_width].reshape(key_rows, kv_heads, HDIM)
        value_part = flat[:, kv_width:].reshape(key_rows, kv_heads, HDIM)

        def attend(unused):
            scores = (
                jnp.einsum(
                    "qhgd,khd->hgqk", query_split, key_part, preferred_element_type=jnp.float32
                )
                * inverse_root
            )
            scores = (
                scores + cum_rows[:, :, :, None] - flat_cum[:, :, None, :] - lse_rows[:, :, :, None]
            )
            allowed = flat_pos[None, :] <= positions[:, None]
            weights = jnp.exp(jnp.where(allowed, scores, NEG_LARGE))
            upstream = jnp.einsum(
                "qhgd,khd->hgqk", cotan_split, value_part, preferred_element_type=jnp.float32
            )
            dscore_low = (weights * (upstream - term_rows[:, :, :, None])).astype(jnp.bfloat16)
            weights_low = weights.astype(jnp.bfloat16)
            query_add = (
                jnp.einsum(
                    "hgqk,khd->qhgd", dscore_low, key_part, preferred_element_type=jnp.float32
                )
                * inverse_root
            )
            key_add = (
                jnp.einsum(
                    "hgqk,qhgd->khd", dscore_low, query_split, preferred_element_type=jnp.float32
                )
                * inverse_root
            )
            value_add = jnp.einsum(
                "hgqk,qhgd->khd", weights_low, cotan_split, preferred_element_type=jnp.float32
            )
            joined = jnp.concatenate(
                [key_add.reshape(key_rows, kv_width), value_add.reshape(key_rows, kv_width)], axis=1
            )
            return (query_add, joined.reshape(count, block_rows, 2 * kv_width))

        def nothing(unused):
            return (
                jnp.zeros((tokens, kv_heads, groups, HDIM), jnp.float32),
                jnp.zeros((count, block_rows, 2 * kv_width), jnp.float32),
            )

        return lax.cond(jnp.min(flat_pos) <= last_row, attend, nothing, 0)

    stacked = jnp.concatenate([keys, values], axis=1)
    query_start = jnp.zeros((tokens, kv_heads, groups, HDIM), jnp.float32)
    copies = jnp.arange(depth)
    turns = devices // depth
    bundle_pieces = [stacked]
    bundle_cums = [cumulative]
    for step in range(1, depth):
        bundle_pieces.append(shifted(stacked, "sp", step))
        bundle_cums.append(shifted(cumulative, "sp", step))

    def turn(turn_index, state_now):
        query_total, bundle, bundle_cum, bundle_grads = state_now
        anchor = (my_index - depth * turn_index) % devices
        blocks = (anchor - copies) % devices
        key_pos = blocks[:, None] * tokens + jnp.arange(tokens)[None, :]
        query_add, grad_add = visit_bundle(bundle, bundle_cum, key_pos)
        bundle = shifted(bundle, "sp", depth)
        bundle_cum, bundle_grads = shifted_2((bundle_cum, bundle_grads + grad_add), "sp", depth)
        return (query_total + query_add, bundle, bundle_cum, bundle_grads)

    start_state = (
        query_start,
        jnp.stack(bundle_pieces),
        jnp.stack(bundle_cums),
        jnp.zeros((depth, tokens, 2 * kv_width), jnp.float32),
    )
    finished = lax.fori_loop(0, turns, turn, start_state)
    query_total = finished[0]
    final_grads = finished[3]
    gradients = final_grads[0]
    for step in range(1, depth):
        gradients = gradients + shifted(final_grads[step], "sp", -step)
    query_grad = query_total.reshape(tokens, head_count * HDIM).astype(jnp.bfloat16)
    key_grad = gradients[:, :kv_width].astype(jnp.bfloat16)
    value_grad = gradients[:, kv_width:].astype(jnp.bfloat16)
    whole_rows = lax.all_gather(normed, "tp", axis=1, tiled=True)
    weight_grad = lax.psum_scatter(
        lax.dot_general(
            whole_rows, key_grad, (((0,), (0,)), ((), ())), preferred_element_type=jnp.float32
        ),
        "sp",
        scatter_dimension=0,
        tiled=True,
    )
    return (query_grad, key_grad, value_grad, weight_grad)


F32, BF16 = (jnp.float32, jnp.bfloat16)
HBM = pl.BlockSpec(memory_space=pl.ANY)
NT = (((1,), (1,)), ((), ()))
NN = (((1,), (0,)), ((), ()))


def dot(a, b, dims=NN, precision=None):
    return lax.dot_general(a, b, dims, precision=precision, preferred_element_type=F32)


def split(x):
    high = x.astype(BF16).astype(F32)
    middle = (x - high).astype(BF16).astype(F32)
    parts = [high, middle, x - high - middle, jnp.zeros_like(x)]
    return jnp.concatenate(parts, axis=0).astype(BF16)


def unsplit(parts):
    wide = parts.astype(F32)
    rows = wide.shape[0] // 4
    return wide[:rows] + wide[rows : 2 * rows] + wide[2 * rows : 3 * rows]


def fused(
    n, m,
    q_hbm, k_hbm, v_hbm, gate_hbm, lse_hbm, out_hbm, cot_hbm, normed_hbm,
    qg_ref, kg_ref, vg_ref, wg_ref,
    q_in, gate_in, lse_in, out_in, cot_in,
    normed_all, kv, sums, diag, dq, grad_send, grad_recv, grad_own, w_send, w_recv,
    in_sem, norm_in_sem, norm_send, norm_recv, kv_send, kv_recv,
    gr_send, gr_recv, wt_send, wt_recv,
):
    me = lax.axis_index("sp")
    tp = lax.axis_index("tp")
    tokens, width = q_in.shape
    groups = gate_in.shape[0]
    span = groups * tokens
    chunk = normed_all.shape[2]
    per = normed_all.shape[0] // m
    scale = HDIM ** (-0.5)

    barrier = pltpu.get_barrier_semaphore()
    for k in range(1, n):
        pl.semaphore_signal(barrier, inc=1, device_id={"sp": lax.rem(me + k, n)}, device_id_type=pl.DeviceIdType.MESH)
    for k in range(1, m):
        pl.semaphore_signal(barrier, inc=1, device_id={"tp": lax.rem(tp + k, m)}, device_id_type=pl.DeviceIdType.MESH)

    pairs = [
        (k_hbm, kv.at[0, pl.ds(0, HDIM)]), (v_hbm, kv.at[0, pl.ds(HDIM, HDIM)]), (gate_hbm, gate_in), (q_hbm, q_in), (cot_hbm, cot_in),
        (out_hbm, out_in), (lse_hbm, lse_in),
    ]
    loads = [pltpu.make_async_copy(a, b, in_sem.at[i]) for i, (a, b) in enumerate(pairs)]
    for load in loads:
        load.start()
    norm_loads = [
        pltpu.make_async_copy(
            normed_hbm.at[:, pl.ds(c * chunk, chunk)], normed_all.at[tp * per + c], norm_in_sem.at[c]
        )
        for c in range(per)
    ]
    for load in norm_loads:
        load.start()

    for load in loads[:3]:
        load.wait()
    rows = lax.broadcasted_iota(jnp.int32, (tokens, tokens), 0)
    cols = lax.broadcasted_iota(jnp.int32, (tokens, tokens), 1)
    gate = gate_in[...]
    local = dot(gate, (rows <= cols).astype(F32), NN, lax.Precision.HIGHEST)
    total = jnp.broadcast_to(jnp.sum(gate, axis=1, keepdims=True), gate.shape)
    kv[0, 2 * HDIM :, :] = split(jnp.concatenate([total - local, total], axis=0))

    for load in loads[3:]:
        load.wait()
    low = lax.broadcasted_iota(jnp.int32, (tokens, 2 * HDIM), 1) < HDIM
    for pair in range(groups // 2):
        lanes = pl.ds(2 * HDIM * pair, 2 * HDIM)
        two = q_in[:, lanes].astype(F32) * scale
        up = cot_in[:, lanes].astype(F32)
        for half in range(2):
            head = 2 * pair + half
            q_head = two if half == 0 else pltpu.roll(two, HDIM, 1)
            c_head = up if half == 1 else pltpu.roll(up, HDIM, 1)
            diag[pl.ds(head * tokens, tokens), :] = jnp.where(low, q_head, 0.0).astype(BF16)
            diag[pl.ds(span + head * tokens, tokens), :] = jnp.where(low, 0.0, c_head).astype(BF16)
    product = out_in[...].astype(F32) * cot_in[...].astype(F32)
    delta = jnp.sum(product.T.reshape(groups, HDIM, tokens), axis=1)
    row_term = local - lse_in[...]

    for load in norm_loads:
        load.wait()
    pl.semaphore_wait(barrier, n - 1 + m - 1)

    def kv_copy(k):
        where = {"sp": lax.rem(me + k, n)}
        return pltpu.make_async_remote_copy(kv.at[0], kv.at[k], kv_send.at[k], kv_recv.at[k], where, pl.DeviceIdType.MESH)

    def norm_copy(k):
        mine = normed_all.at[pl.ds(tp * per, per)]
        return pltpu.make_async_remote_copy(
            mine, mine, norm_send.at[k], norm_recv.at[k], {"tp": lax.rem(tp + k, m)}, pl.DeviceIdType.MESH
        )

    def norm_arrival(k):
        theirs = normed_all.at[pl.ds(lax.rem(tp + m - k, m) * per, per)]
        return pltpu.make_async_remote_copy(
            theirs, theirs, norm_send.at[k], norm_recv.at[k], {"tp": lax.rem(tp + k, m)}, pl.DeviceIdType.MESH
        )

    def grad_copy(k):
        where = {"sp": lax.rem(me + n - k, n)}
        return pltpu.make_async_remote_copy(
            grad_send.at[k], grad_recv.at[k], gr_send.at[k], gr_recv.at[k], where, pl.DeviceIdType.MESH
        )

    def weight_copy(there):
        return pltpu.make_async_remote_copy(
            w_send.at[there], w_recv.at[me], wt_send.at[there], wt_recv.at[me], {"sp": there}, pl.DeviceIdType.MESH
        )

    def weight_arrival(there):
        return pltpu.make_async_remote_copy(
            w_send.at[there], w_recv.at[there], wt_send.at[there], wt_recv.at[there], {"sp": there}, pl.DeviceIdType.MESH
        )

    def far_first(step):
        step = step + jnp.where(step >= jnp.where(2 * me < n, n - 1 - me, me), 1, 0)
        return jnp.where(2 * me < n, n - 1 - step, step)

    for k in range(1, n):
        @pl.when(me + k < n)
        def _(k=k):
            kv_copy(k).start()
    for k in range(1, m):
        norm_copy(k).start()

    def visit(k, key_rows):
        block = kv[k, 0 : 2 * HDIM, :]
        both = dot(block.T, diag[...], NT)
        key_cols = key_rows.T
        prob_parts, score_parts = ([], [])
        for h in range(groups):
            score = both[:, h * tokens : (h + 1) * tokens] + (row_term[h : h + 1, :] + key_cols[:, h : h + 1])
            if k == 0:
                score = jnp.where(rows <= cols, score, NEG_LARGE)
            prob = jnp.exp(score)
            dprob = both[:, span + h * tokens : span + (h + 1) * tokens]
            prob_parts.append(prob.astype(BF16))
            score_parts.append((prob * (dprob - delta[h : h + 1, :])).astype(BF16))
        dscore = jnp.concatenate(score_parts, axis=1)
        weights = jnp.concatenate(score_parts + prob_parts, axis=1)
        grads = dot(weights, diag[...])
        dq_add = dot(block[:HDIM, :], dscore)
        if k == 0:
            dq[...] = dq_add
            grad_own[...] = grads
        else:
            dq[...] += dq_add
            grad_send[k] = grads.astype(BF16)

    visit(0, jnp.concatenate([-local, -local], axis=0))

    for k in range(1, n):
        @pl.when(k <= me)
        def _(k=k):
            kv_copy(k).wait_recv()
            sums[k] = unsplit(kv[k, 2 * HDIM :, :])
            key_rows = sums[k, 0:groups, :]
            for between in range(1, k):
                key_rows = key_rows + sums[between, groups:, :]
            visit(k, jnp.concatenate([key_rows, key_rows], axis=0))
            grad_copy(k).start()

    for pair in range(groups // 2):
        first = dq[:, pl.ds(2 * pair * tokens, tokens)]
        second = dq[:, pl.ds((2 * pair + 1) * tokens, tokens)]
        joined = jnp.concatenate([first, second], axis=0) * scale
        qg_ref[:, pl.ds(2 * HDIM * pair, 2 * HDIM)] = joined.T.astype(BF16)

    for k in range(1, n):
        @pl.when(me + k < n)
        def _(k=k):
            grad_copy(k).wait_recv()
            grad_own[...] += grad_recv[k].astype(F32)
    grads = grad_own[...].T.astype(BF16)
    key_grad_t = grads[:HDIM, :]
    kg_ref[...] = key_grad_t
    vg_ref[...] = grads[HDIM:, :]

    for k in range(1, m):
        norm_arrival(k).wait_recv()
    for k in range(n - 1):
        there = far_first(k)
        w_send[there] = dot(key_grad_t, normed_all[there]).astype(BF16)
        weight_copy(there).start()
    weight = dot(key_grad_t, normed_all[me])
    for k in range(n - 2, -1, -1):
        there = far_first(k)
        weight_arrival(there).wait_recv()
        weight = weight + w_recv[there].astype(F32)
    wg_ref[...] = weight

    for k in range(1, m):
        norm_copy(k).wait_send()
    for k in range(1, n):
        weight_copy(far_first(k - 1)).wait_send()

        @pl.when(me + k < n)
        def _(k=k):
            kv_copy(k).wait_send()

        @pl.when(k <= me)
        def _(k=k):
            grad_copy(k).wait_send()


def hand_over(*refs):
    count = len(refs) // 2
    sems = refs[-1]
    copies = [pltpu.make_async_copy(refs[i], refs[count + i], sems.at[i]) for i in range(count)]
    for copy in copies:
        copy.start()
    for copy in copies:
        copy.wait()


def one_kernel(n, m, queries, keys, values, log_gate, log_sum, output, cotangent, normed):
    tokens, width = queries.shape
    kv_width = keys.shape[1]
    groups = log_gate.shape[0]
    per = n // m
    chunk = normed.shape[1] // per
    pair = 2 * HDIM
    vmem = pltpu.VMEM
    dma = pltpu.SemaphoreType.DMA
    full = pl.BlockSpec(memory_space=pltpu.VMEM)
    shapes = (
        ((tokens, width), BF16), ((kv_width, tokens), BF16), ((kv_width, tokens), BF16), ((kv_width, chunk), F32)
    )
    results = pl.pallas_call(
            functools.partial(fused, n, m),
            out_shape=tuple(vmem(*shape) for shape in shapes),
            in_specs=[HBM] * 8,
            out_specs=(full,) * 4,
            scratch_shapes=[
                vmem((tokens, width), BF16),
                vmem((groups, tokens), F32), vmem((groups, tokens), F32),
                vmem((tokens, width), BF16), vmem((tokens, width), BF16),
                vmem((n, tokens, chunk), BF16), vmem((n, pair + 8 * groups, tokens), BF16), vmem((n, 2 * groups, tokens), F32),
                vmem((2 * groups * tokens, pair), BF16), vmem((HDIM, groups * tokens), F32),
                vmem((n, tokens, pair), BF16), vmem((n, tokens, pair), BF16), vmem((tokens, pair), F32),
                vmem((n, HDIM, chunk), BF16), vmem((n, HDIM, chunk), BF16),
                dma((7,)), dma((per,)), dma((m,)), dma((m,)), dma((n,)), dma((n,)),
                dma((n,)), dma((n,)), dma((n,)), dma((n,)),
            ],
            compiler_params=pltpu.CompilerParams(collective_id=0, has_side_effects=True),
        )(queries, keys.T, values.T, log_gate, log_sum, output, cotangent, normed)
    results = [pltpu.with_memory_space_constraint(x, pltpu.VMEM) for x in results]
    query_grad, key_grad, value_grad, weight_grad = pl.pallas_call(
        hand_over,
        out_shape=tuple(jax.ShapeDtypeStruct(*shape) for shape in shapes),
        in_specs=[full] * 4,
        out_specs=(HBM,) * 4,
        scratch_shapes=[dma((4,))],
    )(*results)
    return (query_grad, key_grad.T, value_grad.T, weight_grad.T)


def chosen(n, m, *arrays):
    queries, keys, log_gate, normed = (arrays[0], arrays[1], arrays[3], arrays[7])
    whole = (
        n % m == 0
        and keys.shape[1] == HDIM
        and log_gate.shape[0] == 4
        and queries.shape[0] == 128
        and normed.shape[1] % (n // m * 128) == 0
    )
    return one_kernel(n, m, *arrays) if whole else body(*arrays)


def solution(mesh):
    n_sp, n_tp = mesh.shape["sp"], mesh.shape["tp"]
    in_specs = (
        P("sp", "tp"),
        P("sp", "tp"),
        P("sp", "tp"),
        P("tp", "sp"),
        P("tp", "sp"),
        P("sp", "tp"),
        P("sp", "tp"),
        P("sp", "tp"),
    )
    out_specs = (P("sp", "tp"), P("sp", "tp"), P("sp", "tp"), P("sp", "tp"))
    return jax.shard_map(functools.partial(chosen, n_sp, n_tp), mesh=mesh, in_specs=in_specs, out_specs=out_specs, check_vma=False)
```

```python
import functools

import jax
import jax.numpy as jnp
from jax import lax
from jax.experimental import pallas as pl
from jax.experimental.pallas import tpu as pltpu
from jax.sharding import PartitionSpec as P

HDIM = 64


NEG_LARGE = -1e30


def prefix(x, axis, combine, identity):
    size, place = (lax.axis_size(axis), lax.axis_index(axis))
    everything = lax.all_gather(x, axis)
    start = jnp.broadcast_to(jnp.asarray(identity, x.dtype), x.shape)

    def hop(k, before):
        reached = k < place
        new = combine(before, everything[k])
        return jnp.where(reached, new, before)

    return lax.fori_loop(0, size, hop, start)


def shifted(x, axis, by):
    size = lax.axis_size(axis)
    pairs = [(i, i + by) for i in range(size) if 0 <= i + by < size]
    return lax.ppermute(x, axis, pairs)


def shifted_2(x, axis, by):
    size = lax.axis_size(axis)
    return lax.ppermute(x, axis, [(i, (i + by) % size) for i in range(size)])


def add_pair(earlier, later):
    return earlier + later


def body(queries, keys, values, log_gate, log_sum, output, cotangent, normed):
    tokens = queries.shape[0]
    head_count = log_gate.shape[0]
    kv_width = keys.shape[1]
    kv_heads = kv_width // HDIM
    groups = head_count // kv_heads
    inverse_root = HDIM ** (-0.5)
    devices = lax.axis_size("sp")
    my_index = lax.axis_index("sp")
    depth = 8
    totals = jnp.sum(log_gate, axis=1)
    before = prefix(totals, "sp", add_pair, jnp.zeros_like(totals))
    cumulative = jnp.cumsum(log_gate, axis=1) + before[:, None]
    row_terms = jnp.sum(
        (output.astype(jnp.float32) * cotangent.astype(jnp.float32)).reshape(
            tokens, head_count, HDIM
        ),
        axis=2,
    ).T
    query_split = queries.reshape(tokens, kv_heads, groups, HDIM)
    cotan_split = cotangent.reshape(tokens, kv_heads, groups, HDIM)
    cum_rows = cumulative.reshape(kv_heads, groups, tokens)
    lse_rows = log_sum.reshape(kv_heads, groups, tokens)
    term_rows = row_terms.reshape(kv_heads, groups, tokens)
    positions = my_index * tokens + jnp.arange(tokens)
    last_row = my_index * tokens + tokens - 1

    def visit_bundle(bundle, bundle_cum, key_pos):
        count = bundle.shape[0]
        block_rows = bundle.shape[1]
        key_rows = count * block_rows
        flat = bundle.reshape(key_rows, 2 * kv_width)
        flat_cum = jnp.transpose(bundle_cum, (1, 0, 2)).reshape(kv_heads, groups, key_rows)
        flat_pos = key_pos.reshape(key_rows)
        key_part = flat[:, :kv_width].reshape(key_rows, kv_heads, HDIM)
        value_part = flat[:, kv_width:].reshape(key_rows, kv_heads, HDIM)

        def attend(unused):
            scores = (
                jnp.einsum(
                    "qhgd,khd->hgqk", query_split, key_part, preferred_element_type=jnp.float32
                )
                * inverse_root
            )
            scores = (
                scores + cum_rows[:, :, :, None] - flat_cum[:, :, None, :] - lse_rows[:, :, :, None]
            )
            allowed = flat_pos[None, :] <= positions[:, None]
            weights = jnp.exp(jnp.where(allowed, scores, NEG_LARGE))
            upstream = jnp.einsum(
                "qhgd,khd->hgqk", cotan_split, value_part, preferred_element_type=jnp.float32
            )
            dscore_low = (weights * (upstream - term_rows[:, :, :, None])).astype(jnp.bfloat16)
            weights_low = weights.astype(jnp.bfloat16)
            query_add = (
                jnp.einsum(
                    "hgqk,khd->qhgd", dscore_low, key_part, preferred_element_type=jnp.float32
                )
                * inverse_root
            )
            key_add = (
                jnp.einsum(
                    "hgqk,qhgd->khd", dscore_low, query_split, preferred_element_type=jnp.float32
                )
                * inverse_root
            )
            value_add = jnp.einsum(
                "hgqk,qhgd->khd", weights_low, cotan_split, preferred_element_type=jnp.float32
            )
            joined = jnp.concatenate(
                [key_add.reshape(key_rows, kv_width), value_add.reshape(key_rows, kv_width)], axis=1
            )
            return (query_add, joined.reshape(count, block_rows, 2 * kv_width))

        def nothing(unused):
            return (
                jnp.zeros((tokens, kv_heads, groups, HDIM), jnp.float32),
                jnp.zeros((count, block_rows, 2 * kv_width), jnp.float32),
            )

        return lax.cond(jnp.min(flat_pos) <= last_row, attend, nothing, 0)

    stacked = jnp.concatenate([keys, values], axis=1)
    query_start = jnp.zeros((tokens, kv_heads, groups, HDIM), jnp.float32)
    copies = jnp.arange(depth)
    turns = devices // depth
    bundle_pieces = [stacked]
    bundle_cums = [cumulative]
    for step in range(1, depth):
        bundle_pieces.append(shifted(stacked, "sp", step))
        bundle_cums.append(shifted(cumulative, "sp", step))

    def turn(turn_index, state_now):
        query_total, bundle, bundle_cum, bundle_grads = state_now
        anchor = (my_index - depth * turn_index) % devices
        blocks = (anchor - copies) % devices
        key_pos = blocks[:, None] * tokens + jnp.arange(tokens)[None, :]
        query_add, grad_add = visit_bundle(bundle, bundle_cum, key_pos)
        bundle = shifted(bundle, "sp", depth)
        bundle_cum, bundle_grads = shifted_2((bundle_cum, bundle_grads + grad_add), "sp", depth)
        return (query_total + query_add, bundle, bundle_cum, bundle_grads)

    start_state = (
        query_start,
        jnp.stack(bundle_pieces),
        jnp.stack(bundle_cums),
        jnp.zeros((depth, tokens, 2 * kv_width), jnp.float32),
    )
    finished = lax.fori_loop(0, turns, turn, start_state)
    query_total = finished[0]
    final_grads = finished[3]
    gradients = final_grads[0]
    for step in range(1, depth):
        gradients = gradients + shifted(final_grads[step], "sp", -step)
    query_grad = query_total.reshape(tokens, head_count * HDIM).astype(jnp.bfloat16)
    key_grad = gradients[:, :kv_width].astype(jnp.bfloat16)
    value_grad = gradients[:, kv_width:].astype(jnp.bfloat16)
    whole_rows = lax.all_gather(normed, "tp", axis=1, tiled=True)
    weight_grad = lax.psum_scatter(
        lax.dot_general(
            whole_rows, key_grad, (((0,), (0,)), ((), ())), preferred_element_type=jnp.float32
        ),
        "sp",
        scatter_dimension=0,
        tiled=True,
    )
    return (query_grad, key_grad, value_grad, weight_grad)


F32, BF16 = (jnp.float32, jnp.bfloat16)
HBM = pl.BlockSpec(memory_space=pl.ANY)
NT = (((1,), (1,)), ((), ()))
NN = (((1,), (0,)), ((), ()))


def dot(a, b, dims=NN, precision=None):
    return lax.dot_general(a, b, dims, precision=precision, preferred_element_type=F32)


def split(x):
    high = x.astype(BF16).astype(F32)
    middle = (x - high).astype(BF16).astype(F32)
    parts = [high, middle, x - high - middle, jnp.zeros_like(x)]
    return jnp.concatenate(parts, axis=0).astype(BF16)


def unsplit(parts):
    wide = parts.astype(F32)
    rows = wide.shape[0] // 4
    return wide[:rows] + wide[rows : 2 * rows] + wide[2 * rows : 3 * rows]


def fused(
    n, m,
    q_hbm, k_hbm, v_hbm, gate_hbm, lse_hbm, out_hbm, cot_hbm, normed_hbm,
    qg_ref, kg_ref, vg_ref, wg_ref,
    q_in, gate_in, lse_in, out_in, cot_in,
    normed_all, kv, sums, diag, dq, grad_send, grad_recv, grad_own, w_send, w_recv,
    in_sem, norm_in_sem, norm_send, norm_recv, kv_send, kv_recv,
    gr_send, gr_recv, wt_send, wt_recv,
):
    me = lax.axis_index("sp")
    tp = lax.axis_index("tp")
    tokens, width = q_in.shape
    groups = gate_in.shape[0]
    span = groups * tokens
    chunk = normed_all.shape[2]
    per = normed_all.shape[0] // m
    scale = HDIM ** (-0.5)

    barrier = pltpu.get_barrier_semaphore()
    for k in range(1, n):
        pl.semaphore_signal(barrier, inc=1, device_id={"sp": lax.rem(me + k, n)}, device_id_type=pl.DeviceIdType.MESH)
    for k in range(1, m):
        pl.semaphore_signal(barrier, inc=1, device_id={"tp": lax.rem(tp + k, m)}, device_id_type=pl.DeviceIdType.MESH)

    pairs = [
        (k_hbm, kv.at[0, pl.ds(0, HDIM)]), (v_hbm, kv.at[0, pl.ds(HDIM, HDIM)]), (gate_hbm, gate_in), (q_hbm, q_in), (cot_hbm, cot_in),
        (out_hbm, out_in), (lse_hbm, lse_in),
    ]
    loads = [pltpu.make_async_copy(a, b, in_sem.at[i]) for i, (a, b) in enumerate(pairs)]
    for load in loads:
        load.start()
    norm_loads = [
        pltpu.make_async_copy(
            normed_hbm.at[:, pl.ds(c * chunk, chunk)], normed_all.at[tp * per + c], norm_in_sem.at[c]
        )
        for c in range(per)
    ]
    for load in norm_loads:
        load.start()

    for load in loads[:3]:
        load.wait()
    rows = lax.broadcasted_iota(jnp.int32, (tokens, tokens), 0)
    cols = lax.broadcasted_iota(jnp.int32, (tokens, tokens), 1)
    gate = gate_in[...]
    local = dot(gate, (rows <= cols).astype(F32), NN, lax.Precision.HIGHEST)
    total = jnp.broadcast_to(jnp.sum(gate, axis=1, keepdims=True), gate.shape)
    kv[0, 2 * HDIM :, :] = split(total - local + gate)

    for load in loads[3:]:
        load.wait()
    low = lax.broadcasted_iota(jnp.int32, (tokens, 2 * HDIM), 1) < HDIM
    for pair in range(groups // 2):
        lanes = pl.ds(2 * HDIM * pair, 2 * HDIM)
        two = q_in[:, lanes].astype(F32) * scale
        up = cot_in[:, lanes].astype(F32)
        for half in range(2):
            head = 2 * pair + half
            q_head = two if half == 0 else pltpu.roll(two, HDIM, 1)
            c_head = up if half == 1 else pltpu.roll(up, HDIM, 1)
            diag[pl.ds(head * tokens, tokens), :] = jnp.where(low, q_head, 0.0).astype(BF16)
            diag[pl.ds(span + head * tokens, tokens), :] = jnp.where(low, 0.0, c_head).astype(BF16)
    product = out_in[...].astype(F32) * cot_in[...].astype(F32)
    delta = jnp.sum(product.T.reshape(groups, HDIM, tokens), axis=1)
    row_term = local - lse_in[...]

    for load in norm_loads:
        load.wait()
    pl.semaphore_wait(barrier, n - 1 + m - 1)

    def kv_copy(k):
        where = {"sp": lax.rem(me + k, n)}
        return pltpu.make_async_remote_copy(kv.at[0], kv.at[k], kv_send.at[k], kv_recv.at[k], where, pl.DeviceIdType.MESH)

    def norm_copy(k):
        mine = normed_all.at[pl.ds(tp * per, per)]
        return pltpu.make_async_remote_copy(
            mine, mine, norm_send.at[k], norm_recv.at[k], {"tp": lax.rem(tp + k, m)}, pl.DeviceIdType.MESH
        )

    def norm_arrival(k):
        theirs = normed_all.at[pl.ds(lax.rem(tp + m - k, m) * per, per)]
        return pltpu.make_async_remote_copy(
            theirs, theirs, norm_send.at[k], norm_recv.at[k], {"tp": lax.rem(tp + k, m)}, pl.DeviceIdType.MESH
        )

    def grad_copy(k):
        where = {"sp": lax.rem(me + n - k, n)}
        return pltpu.make_async_remote_copy(
            grad_send.at[k], grad_recv.at[k], gr_send.at[k], gr_recv.at[k], where, pl.DeviceIdType.MESH
        )

    def weight_copy(there):
        return pltpu.make_async_remote_copy(
            w_send.at[there], w_recv.at[me], wt_send.at[there], wt_recv.at[me], {"sp": there}, pl.DeviceIdType.MESH
        )

    def weight_arrival(there):
        return pltpu.make_async_remote_copy(
            w_send.at[there], w_recv.at[there], wt_send.at[there], wt_recv.at[there], {"sp": there}, pl.DeviceIdType.MESH
        )

    def partner(step):
        return lax.rem(me + n - 1 - step, n)

    for k in range(1, n):
        @pl.when(me + k < n)
        def _(k=k):
            kv_copy(k).start()
    for k in range(1, m):
        norm_copy(k).start()

    last = lax.broadcasted_iota(jnp.int32, (groups, tokens), 1) == tokens - 1

    def visit(k, key_rows):
        block = kv[k, 0 : 2 * HDIM, :]
        both = dot(block.T, diag[...], NT)
        key_cols = key_rows.T
        prob_parts, score_parts = ([], [])
        for h in range(groups):
            score = both[:, h * tokens : (h + 1) * tokens] + (row_term[h : h + 1, :] + key_cols[:, h : h + 1])
            if k == 0:
                score = jnp.where(rows <= cols, score, NEG_LARGE)
            prob = jnp.exp(score)
            dprob = both[:, span + h * tokens : span + (h + 1) * tokens]
            prob_parts.append(prob.astype(BF16))
            score_parts.append((prob * (dprob - delta[h : h + 1, :])).astype(BF16))
        dscore = jnp.concatenate(score_parts, axis=1)
        weights = jnp.concatenate(score_parts + prob_parts, axis=1)
        grads = dot(weights, diag[...])
        dq_add = dot(block[:HDIM, :], dscore)
        if k == 0:
            dq[...] = dq_add
            grad_own[...] = grads
        else:
            dq[...] += dq_add
            grad_send[k] = grads.astype(BF16)

    visit(0, jnp.concatenate([-local, -local], axis=0))

    for k in range(1, n):
        @pl.when(k <= me)
        def _(k=k):
            kv_copy(k).wait_recv()
            after = unsplit(kv[k, 2 * HDIM :, :])
            past = pltpu.roll(jnp.concatenate([after, after], axis=0), tokens - 1, 1)[:groups]
            sums[k, 0:groups, :] = jnp.where(last, 0.0, past)
            sums[k, groups:, :] = jnp.broadcast_to(after[:, 0:1], after.shape)
            key_rows = sums[k, 0:groups, :]
            for between in range(1, k):
                key_rows = key_rows + sums[between, groups:, :]
            visit(k, jnp.concatenate([key_rows, key_rows], axis=0))
            grad_copy(k).start()

    for pair in range(groups // 2):
        first = dq[:, pl.ds(2 * pair * tokens, tokens)]
        second = dq[:, pl.ds((2 * pair + 1) * tokens, tokens)]
        joined = jnp.concatenate([first, second], axis=0) * scale
        qg_ref[:, pl.ds(2 * HDIM * pair, 2 * HDIM)] = joined.T.astype(BF16)

    for k in range(1, n):
        @pl.when(me + k < n)
        def _(k=k):
            grad_copy(k).wait_recv()
            grad_own[...] += grad_recv[k].astype(F32)
    grads = grad_own[...].T.astype(BF16)
    key_grad_t = grads[:HDIM, :]
    kg_ref[...] = key_grad_t
    vg_ref[...] = grads[HDIM:, :]

    for k in range(1, m):
        norm_arrival(k).wait_recv()
    for k in range(n - 1):
        there = partner(k)
        w_send[there] = dot(key_grad_t, normed_all[there]).astype(BF16)
        weight_copy(there).start()
    weight = dot(key_grad_t, normed_all[me])
    for k in range(n - 2, -1, -1):
        there = partner(k)
        weight_arrival(there).wait_recv()
        weight = weight + w_recv[there].astype(F32)
    wg_ref[...] = weight

    for k in range(1, m):
        norm_copy(k).wait_send()
    for k in range(1, n):
        weight_copy(partner(k - 1)).wait_send()

        @pl.when(me + k < n)
        def _(k=k):
            kv_copy(k).wait_send()

        @pl.when(k <= me)
        def _(k=k):
            grad_copy(k).wait_send()


def hand_over(*refs):
    count = len(refs) // 2
    sems = refs[-1]
    copies = [pltpu.make_async_copy(refs[i], refs[count + i], sems.at[i]) for i in range(count)]
    for copy in copies:
        copy.start()
    for copy in copies:
        copy.wait()


def one_kernel(n, m, queries, keys, values, log_gate, log_sum, output, cotangent, normed):
    tokens, width = queries.shape
    kv_width = keys.shape[1]
    groups = log_gate.shape[0]
    per = n // m
    chunk = normed.shape[1] // per
    pair = 2 * HDIM
    vmem = pltpu.VMEM
    dma = pltpu.SemaphoreType.DMA
    full = pl.BlockSpec(memory_space=pltpu.VMEM)
    shapes = (
        ((tokens, width), BF16), ((kv_width, tokens), BF16), ((kv_width, tokens), BF16), ((kv_width, chunk), F32)
    )
    results = pl.pallas_call(
            functools.partial(fused, n, m),
            out_shape=tuple(vmem(*shape) for shape in shapes),
            in_specs=[HBM] * 8,
            out_specs=(full,) * 4,
            scratch_shapes=[
                vmem((tokens, width), BF16),
                vmem((groups, tokens), F32), vmem((groups, tokens), F32),
                vmem((tokens, width), BF16), vmem((tokens, width), BF16),
                vmem((n, tokens, chunk), BF16), vmem((n, pair + 4 * groups, tokens), BF16), vmem((n, 2 * groups, tokens), F32),
                vmem((2 * groups * tokens, pair), BF16), vmem((HDIM, groups * tokens), F32),
                vmem((n, tokens, pair), BF16), vmem((n, tokens, pair), BF16), vmem((tokens, pair), F32),
                vmem((n, HDIM, chunk), BF16), vmem((n, HDIM, chunk), BF16),
                dma((7,)), dma((per,)), dma((m,)), dma((m,)), dma((n,)), dma((n,)),
                dma((n,)), dma((n,)), dma((n,)), dma((n,)),
            ],
            compiler_params=pltpu.CompilerParams(collective_id=0, has_side_effects=True),
        )(queries, keys.T, values.T, log_gate, log_sum, output, cotangent, normed)
    results = [pltpu.with_memory_space_constraint(x, pltpu.VMEM) for x in results]
    query_grad, key_grad, value_grad, weight_grad = pl.pallas_call(
        hand_over,
        out_shape=tuple(jax.ShapeDtypeStruct(*shape) for shape in shapes),
        in_specs=[full] * 4,
        out_specs=(HBM,) * 4,
        scratch_shapes=[dma((4,))],
    )(*results)
    return (query_grad, key_grad.T, value_grad.T, weight_grad.T)


def chosen(n, m, *arrays):
    queries, keys, log_gate, normed = (arrays[0], arrays[1], arrays[3], arrays[7])
    whole = (
        n % m == 0
        and keys.shape[1] == HDIM
        and log_gate.shape[0] == 4
        and queries.shape[0] == 128
        and normed.shape[1] % (n // m * 128) == 0
    )
    return one_kernel(n, m, *arrays) if whole else body(*arrays)


def solution(mesh):
    n_sp, n_tp = mesh.shape["sp"], mesh.shape["tp"]
    in_specs = (
        P("sp", "tp"),
        P("sp", "tp"),
        P("sp", "tp"),
        P("tp", "sp"),
        P("tp", "sp"),
        P("sp", "tp"),
        P("sp", "tp"),
        P("sp", "tp"),
    )
    out_specs = (P("sp", "tp"), P("sp", "tp"), P("sp", "tp"), P("sp", "tp"))
    return jax.shard_map(functools.partial(chosen, n_sp, n_tp), mesh=mesh, in_specs=in_specs, out_specs=out_specs, check_vma=False)
```
